32 devices in a mesh: sp: 8 (over z, y), dp: 4 (over x, core).
Axes of the slice: x: 2, y: 2, z: 4, core: 2. Of those that a mesh axis runs over, the one named last changes fastest.
Arguments:
- queries: bfloat16 [16, 16, 512, 128], P('dp', None, 'sp'), may hold values from -6 to 6
- key_maps: bfloat16 [16, 16, 512, 128], P('dp', None, 'sp'), may hold values from -6 to 6
- value_rows: bfloat16 [16, 16, 512, 128], P('dp', None, 'sp'), may hold values from -6 to 6
- gate_logits: bfloat16 [512, 16, 2048], P('sp', 'dp'), may hold values from -6 to 6
- mix_lambda: float32 [16], replicated, may hold values from 0.3 to 0.8
- head_gain: float32 [128], replicated, may hold values from 0.1 to 1.9
- out_weight: bfloat16 [2048, 2048], P('sp', 'dp'), may hold values from -0.125 to 0.125
Outputs:
- projected: bfloat16 [512, 16, 2048], P('sp', 'dp')
The draws below stay inside these ranges and needn't reach their ends.
All inputs are finite; a program needn't handle non-finite values.
Results may differ from the reference program's by a relative error of at most 0.0075.
Values may be sent and summed in bfloat16 or wider, within the bound.
A program may use at most 64 MiB of HBM per device.

```python
from functools import partial
import jax
import jax.numpy as jnp
from jax import lax

HEADS = 16
HEAD_DIM = 64
V_DIM = 128
STRETCH = 64
BLOCK = 512
D = 2048
LENGTH = 512
BATCH = 16


def draw_pair(key):
    shape = (BATCH, HEADS, LENGTH, 2 * HEAD_DIM)
    query_key = jax.random.fold_in(key, 11)
    keymap_key = jax.random.fold_in(key, 12)
    query_vals = jnp.clip(1.3 * jax.random.normal(query_key, shape, jnp.float32), -6.0, 6.0)
    keymap_vals = jnp.clip(1.3 * jax.random.normal(keymap_key, shape, jnp.float32), -6.0, 6.0)
    return (query_vals, keymap_vals)


def draw_queries(key, part):
    return draw_pair(key)[0].astype(jnp.bfloat16)


def draw_key_maps(key, part):
    return draw_pair(key)[1].astype(jnp.bfloat16)


def levels(stream_key, extent, shards, smallest, largest):
    factor_of, own = 1.0, jax.random.fold_in(stream_key, 6)
    for position, parts in shards:
        draws = jnp.exp(jax.random.uniform(jax.random.fold_in(own, position), (parts,), jnp.float32, smallest / len(shards), largest / len(shards)))
        factor_of = factor_of * jnp.repeat(draws, extent[position] // parts).reshape([-1 if axis == position else 1 for axis in range(len(extent))])
    return factor_of


def scatter_about(stream_key, shape, spread, reach, pieces=(), dtype=jnp.bfloat16):
    entries = spread * jax.random.normal(stream_key, shape, jnp.float32)
    if pieces:
        entries = entries * levels(stream_key, shape, pieces, -0.22, 0.18)
    return jnp.clip(entries, -reach, reach).astype(dtype)


def setup_inputs(seed: int = 0) -> dict:
    key_of = jax.random.split(jax.random.key(seed), 8)
    queries = draw_queries(jax.random.fold_in(key_of[7], 71), 0)
    key_maps = draw_key_maps(jax.random.fold_in(key_of[7], 71), 0)
    value_rows = scatter_about(key_of[2], (BATCH, HEADS, LENGTH, V_DIM), 1.0, 6.0, ((0, 4), (2, 8)))
    gate_logits = scatter_about(key_of[3], (LENGTH, BATCH, D), 1.0, 6.0, ((0, 8), (1, 4)))
    mix_lambda = jnp.clip(jax.random.uniform(key_of[4], (HEADS,), jnp.float32, 0.3, 0.8), 0.3, 0.8)
    head_gain = jnp.clip(1.0 + 0.18 * jax.random.normal(key_of[5], (V_DIM,), jnp.float32), 0.1, 1.9)
    out_weight = scatter_about(key_of[6], (D, D), D ** -0.5, 0.125, ((0, 8), (1, 4)))
    return dict(queries=queries, key_maps=key_maps, value_rows=value_rows, gate_logits=gate_logits, mix_lambda=mix_lambda, head_gain=head_gain, out_weight=out_weight)


def attend_item(operands, segment_ids, head_gain):
    query_item, key_item, value_item, weight_two = operands
    block_len = min(BLOCK, LENGTH)
    score_scale = HEAD_DIM ** (-0.5)
    outputs = []
    for block_index in range(LENGTH // block_len):
        offset = block_index * block_len
        limit = offset + block_len
        query_rows = query_item[offset:limit]
        key_block = key_item[:limit]
        value_block = value_item[:limit]
        visible = segment_ids[None, :limit] <= segment_ids[offset:limit, None]
        mapped = []
        for which in range(2):
            column_span = slice(which * HEAD_DIM, (which + 1) * HEAD_DIM)
            scores = jnp.dot(query_rows[:, column_span], key_block[:, column_span].T, preferred_element_type=jnp.float32) * score_scale
            scores = jnp.where(visible, scores, -1e+30)
            weights = jnp.exp(scores - lax.optimization_barrier(jnp.max(scores, axis=1, keepdims=True)))
            summed = lax.optimization_barrier(jnp.sum(weights, axis=1, keepdims=True))
            product = jnp.dot(weights.astype(jnp.bfloat16), value_block, preferred_element_type=jnp.float32)
            mapped.append(product / summed)
        combined = mapped[0] - weight_two * mapped[1]
        mean_sq = lax.optimization_barrier(jnp.mean(combined * combined, axis=1, keepdims=True))
        outputs.append((combined * lax.rsqrt(mean_sq + 1e-05) * head_gain).astype(jnp.bfloat16))
    return jnp.concatenate(outputs, axis=0)

def reference(queries, key_maps, value_rows, gate_logits, mix_lambda, head_gain, out_weight):
    item_count = BATCH * HEADS
    segment_ids = (jnp.arange(LENGTH) // STRETCH).astype(jnp.int32)
    lambda_items = jnp.tile(mix_lambda, BATCH)
    normed = lax.map(partial(attend_item, segment_ids=segment_ids, head_gain=head_gain), (queries.reshape(item_count, LENGTH, 2 * HEAD_DIM), key_maps.reshape(item_count, LENGTH, 2 * HEAD_DIM), value_rows.reshape(item_count, LENGTH, V_DIM), lambda_items))
    by_token = jnp.transpose(normed.reshape(BATCH, HEADS, LENGTH, V_DIM), (2, 0, 1, 3)).reshape(LENGTH, BATCH, D)
    gated = (jax.nn.sigmoid(gate_logits.astype(jnp.float32)) * by_token.astype(jnp.float32)).astype(jnp.bfloat16)
    output = jnp.dot(gated.reshape(LENGTH * BATCH, D), out_weight, preferred_element_type=jnp.float32)
    return output.astype(jnp.bfloat16).reshape(LENGTH, BATCH, D)
```

```python
import functools

import jax
import jax.numpy as jnp
from jax import lax
from jax.experimental import pallas as pl
from jax.experimental.pallas import tpu as pltpu
from jax.sharding import PartitionSpec as P

HEAD_DIM = 64
STRETCH = 64
LOG2E = 1.4426950408889634
WINDOW = 8


def plan(n, items):
    rows = items // (n // 4)
    singles = 2 * ((rows * 7) // 32)
    doubles = rows - singles
    outer_single = singles * 2 // 7
    inner_double = doubles // 6
    groups = [
        (outer_single, 0, 0),
        (singles - outer_single, 0, 1),
        (doubles - inner_double, 1, 0),
        (inner_double, 1, 1),
    ]
    order = sorted(
        ((i + 0.5) / count, g) for g, (count, _, _) in enumerate(groups) for i in range(count)
    )
    kinds, lows, highs, seen = [], [], [], 0
    for _, g in order:
        _, kind, low = groups[g]
        kinds.append(kind)
        lows.append(low)
        highs.append(2 + seen % 2)
        seen += kind
    return kinds, lows, highs


def pick(table, index):
    value = jnp.int32(table[0])
    for i, entry in enumerate(table[1:], 1):
        value = jnp.where(index == i, entry, value)
    return value


def attend(q, k, v, start, weight_two, gain, store):
    rows_all, cols = q.shape
    block = min(2 * STRETCH, rows_all)
    factor = HEAD_DIM ** (-0.5) * LOG2E
    first_map = lax.broadcasted_iota(jnp.int32, (block, cols), 1) < cols // 2
    row_seg = (lax.broadcasted_iota(jnp.int32, (2 * block, block), 0) % block) // STRETCH
    col_seg = lax.broadcasted_iota(jnp.int32, (2 * block, block), 1) // STRETCH
    visible = col_seg <= row_seg
    for at in range(0, rows_all, block):
        lo = start + at
        hi = lo + block
        rows = q[at : at + block]
        zero = jnp.zeros_like(rows)
        both = jnp.concatenate([jnp.where(first_map, rows, zero), jnp.where(first_map, zero, rows)], axis=0)
        scores = lax.dot_general(
            both, k[:hi], (((1,), (1,)), ((), ())), preferred_element_type=jnp.float32
        )
        diag = jnp.where(visible, scores[:, lo:], -1e30)
        scores = jnp.concatenate([scores[:, :lo], diag], axis=1) if lo else diag
        highest = jnp.max(scores, axis=1, keepdims=True)
        weights = jnp.exp2((scores - highest) * factor)
        summed = jnp.sum(weights, axis=1, keepdims=True)
        mapped = (
            jnp.dot(weights.astype(jnp.bfloat16), v[:hi], preferred_element_type=jnp.float32) / summed
        )
        combined = mapped[:block] - weight_two * mapped[block:]
        mean_sq = jnp.mean(combined * combined, axis=1, keepdims=True)
        store(at, (combined * lax.rsqrt(mean_sq + 1e-05) * gain).astype(jnp.bfloat16))


def layer_kernel(
    n, m, heads, q_ref, k_ref, v_ref, gate_ref, lam_ref, gain_ref, w_ref, out_ref,
    recv, staged, ret, wbuf, gate_v, gated,
    recv_sem, send_sem, ret_sem, back_sem, w_sem, w_send_sem, gate_sem,
):
    me = lax.axis_index("sp")
    col = lax.axis_index("dp")
    items, toks, cols = q_ref.shape
    seqs = items // heads
    half = n // 2
    quarter = n // 4
    rows = items // quarter
    kinds, lows, highs = plan(n, items)
    low = me < half
    my_quarter = me // quarter
    my_column = lax.rem(me, quarter)
    w_rows, w_cols = w_ref.shape

    cores = 2 if m % 2 == 0 else 1
    xs = m // cores
    ys = 1
    while 2 * (2 * ys) ** 2 <= n:
        ys *= 2
    zs = n // ys
    hz = zs // 2
    my_z, my_y = me // ys, lax.rem(me, ys)
    my_x, my_core = col // cores, lax.rem(col, cores)

    barrier = pltpu.get_barrier_semaphore()

    def greet_sp(step, carry):
        pl.semaphore_signal(barrier, inc=1, device_id={"sp": lax.rem(me + step, n)})
        return carry

    def greet_dp(step, carry):
        pl.semaphore_signal(barrier, inc=1, device_id={"dp": lax.rem(col + step, m)})
        return carry

    gate_copy = pltpu.make_async_copy(gate_ref, gate_v, gate_sem)
    gate_copy.start()
    lax.fori_loop(1, n, greet_sp, 0)
    lax.fori_loop(1, m, greet_dp, 0)

    def w_at(s, d):
        return wbuf.at[d, pl.ds(pl.multiple_of(s * w_rows, w_rows), w_rows)]

    pltpu.make_async_copy(w_ref, w_at(me, col), w_sem.at[me, col]).start()
    pl.semaphore_wait(barrier, n - 1 + m - 1)

    def w_send(src, s, d, **target):
        pltpu.make_async_remote_copy(
            src_ref=src, dst_ref=w_at(s, d), send_sem=w_send_sem, recv_sem=w_sem.at[s, d], device_id=target
        ).start()

    def w_wait(s, d):
        pltpu.make_async_copy(w_at(s, d), w_at(s, d), w_sem.at[s, d]).wait()

    def to_half_peers(src, s, d):
        for i in range(1, hz):
            base = (my_z // hz) * hz
            w_send(src, s, d, sp=(base + lax.rem(my_z - base + i, hz)) * ys + my_y)

    def to_ys(src, s, d):
        for i in range(1, ys):
            w_send(src, s, d, sp=my_z * ys + lax.rem(my_y + i, ys))

    def to_xs(src, s, d):
        for i in range(1, xs):
            w_send(src, s, d, dp=lax.rem(my_x + i, xs) * cores + my_core)

    def to_core(src, s, d):
        if cores > 1:
            w_send(src, s, d, dp=my_x * cores + (1 - my_core))

    base_z = (my_z // hz) * hz
    far_z = hz - base_z
    is_gate = my_z == jnp.where(low, hz - 1, hz)

    w_send(w_ref, me, col, sp=jnp.where(low, hz, hz - 1) * ys + my_y)
    to_half_peers(w_ref, me, col)
    to_ys(w_ref, me, col)
    to_xs(w_ref, me, col)
    to_core(w_ref, me, col)

    def w_near():
        for i in range(1, ys):
            s = my_z * ys + lax.rem(my_y + i, ys)
            w_wait(s, col)
            to_xs(w_at(s, col), s, col)
            to_core(w_at(s, col), s, col)
        for i in range(1, hz):
            s = (base_z + lax.rem(my_z - base_z + i, hz)) * ys + my_y
            w_wait(s, col)
            to_ys(w_at(s, col), s, col)
            to_xs(w_at(s, col), s, col)
            to_core(w_at(s, col), s, col)

    def w_far(gateway):
        for i in range(hz):
            s = (far_z + i) * ys + my_y
            w_wait(s, col)
            if gateway:
                to_half_peers(w_at(s, col), s, col)
            to_ys(w_at(s, col), s, col)
            to_xs(w_at(s, col), s, col)
            to_core(w_at(s, col), s, col)

    def w_side():
        for j in range(1, ys):
            for i in range(1, zs):
                s = lax.rem(my_z + i, zs) * ys + lax.rem(my_y + j, ys)
                w_wait(s, col)
                to_xs(w_at(s, col), s, col)
                to_core(w_at(s, col), s, col)

    def w_across():
        for i in range(1, xs):
            d = lax.rem(my_x + i, xs) * cores + my_core

            def forward(s, carry):
                w_wait(s, d)
                to_core(w_at(s, d), s, d)
                return carry

            lax.fori_loop(0, n, forward, 0)

    def w_last():
        if cores > 1:
            for i in range(xs):
                d = i * cores + (1 - my_core)

                def arrive(s, carry):
                    w_wait(s, d)
                    return carry

                lax.fori_loop(0, n, arrive, 0)
        w_wait(me, col)

    near = 1 + (hz - 1) + (ys - 1) + (xs - 1) + (cores - 1)
    passed = (n - 1) * (xs - 1 + cores - 1) + (zs - 1) * (ys - 1) + n * (xs - 1) * (cores - 1)
    w_sends = near + passed + jnp.where(is_gate, hz * (hz - 1), 0)

    def send_row(r):
        kind, low_q, high_q = pick(kinds, r), pick(lows, r), pick(highs, r)

        def send_item(c, carry):
            item = r * quarter + c
            first = jnp.where((kind == 0) | low, low_q, high_q) * quarter + c

            @pl.when(first == me)
            def _():
                for which, ref in enumerate((q_ref, k_ref, v_ref)):
                    pltpu.make_async_copy(ref.at[item], recv.at[r, which * n + me], recv_sem.at[r]).start()

            def far(which, ref, peer):
                pltpu.make_async_remote_copy(
                    src_ref=ref.at[item],
                    dst_ref=recv.at[r, which * n + me],
                    send_sem=send_sem,
                    recv_sem=recv_sem.at[r],
                    device_id={"sp": peer},
                ).start()

            @pl.when(first != me)
            def _():
                for which, ref in enumerate((q_ref, k_ref, v_ref)):
                    far(which, ref, first)

            @pl.when((kind == 1) & low)
            def _():
                far(1, k_ref, high_q * quarter + c)
                far(2, v_ref, high_q * quarter + c)

            return carry

        lax.fori_loop(0, quarter, send_item, 0)

    def send_first(r, carry):
        send_row(r)
        return carry

    lax.fori_loop(0, min(WINDOW, rows), send_first, 0)
    w_near()

    gain = gain_ref[...]

    def arrived(part, sem):
        pltpu.make_async_copy(part, part, sem).wait()

    def work_row(r, carry):
        @pl.when(r + WINDOW < rows)
        def _():
            send_row(r + WINDOW)

        kind, low_q, high_q = pick(kinds, r), pick(lows, r), pick(highs, r)
        item = r * quarter + my_column
        weight_two = lam_ref[lax.rem(item, heads)]
        is_low = low & (low_q == my_quarter)
        is_high = jnp.logical_not(low) & (kind == 1) & (high_q == my_quarter)

        def part(first, count):
            q = recv[r, first : first + count].reshape(count * toks, cols)
            k = recv[r, n : n + first + count].reshape((first + count) * toks, cols)
            v = recv[r, 2 * n : 2 * n + first + count].reshape((first + count) * toks, cols)

            def store(at, block):
                for i in range(0, block.shape[0], toks):
                    staged[r, first + (at + i) // toks] = block[i : i + toks]

            attend(q, k, v, first * toks, weight_two, gain, store)
            for s in range(first, first + count):

                @pl.when(me == s)
                def _():
                    pltpu.make_async_copy(staged.at[r, s], ret.at[item], ret_sem).start()

                @pl.when(me != s)
                def _():
                    pltpu.make_async_remote_copy(
                        src_ref=staged.at[r, s],
                        dst_ref=ret.at[item],
                        send_sem=back_sem,
                        recv_sem=ret_sem,
                        device_id={"sp": s},
                    ).start()

        @pl.when(is_low & (kind == 0))
        def _():
            arrived(recv.at[r], recv_sem.at[r])

        @pl.when(is_low & (kind == 1))
        def _():
            arrived(recv.at[r, pl.ds(0, 3 * half)], recv_sem.at[r])

        @pl.when(is_high)
        def _():
            arrived(recv.at[r, pl.ds(half, 3 * n - half)], recv_sem.at[r])

        @pl.when(is_low)
        def _():
            part(0, half)

        @pl.when((is_low & (kind == 0)) | is_high)
        def _():
            part(half, half)

        @pl.when((r == rows // 16) & is_gate)
        def _():
            w_far(True)

        @pl.when((r == rows // 4) & jnp.logical_not(is_gate))
        def _():
            w_far(False)

        @pl.when(r == rows // 2)
        def _():
            w_side()

        @pl.when(r == rows - rows // 4)
        def _():
            w_across()

        return carry

    lax.fori_loop(0, rows, work_row, 0)
    w_last()

    n_single = [sum(1 for k, l in zip(kinds, lows) if k == 0 and l == i) for i in range(2)]
    n_double = [sum(1 for k, l in zip(kinds, lows) if k == 1 and l == i) for i in range(2)]
    n_high = [sum(1 for k, h in zip(kinds, highs) if k == 1 and h == i) for i in (2, 3)]
    doubles = sum(kinds) * quarter
    mine = [n_single[i] + n_double[i] for i in range(2)] + n_high
    sent = items - pick(mine, my_quarter)
    backs = pick(
        [mine[i] * (half - 1) + n_single[i] * half for i in range(2)] + [h * (half - 1) for h in n_high],
        my_quarter,
    )

    def drain(part, sem, count):
        def one(i, carry):
            pltpu.make_async_copy(part, part, sem).wait()
            return carry

        lax.fori_loop(0, count, one, 0)

    drain(recv.at[0, pl.ds(0, 3)], send_sem, sent)
    drain(recv.at[0, pl.ds(0, 2)], send_sem, jnp.where(low, doubles, 0))
    drain(w_at(me, col), w_send_sem, w_sends)

    gate_copy.wait()
    pltpu.make_async_copy(ret, ret, ret_sem).wait()
    for s in range(seqs):
        for h in range(heads):
            logits = gate_v[:, s, h * cols : (h + 1) * cols].astype(jnp.float32)
            gated[s * toks : (s + 1) * toks, h * cols : (h + 1) * cols] = (
                jax.nn.sigmoid(logits) * ret[s * heads + h].astype(jnp.float32)
            ).astype(jnp.bfloat16)
    for d in range(m):
        result = jnp.dot(gated[...], wbuf[d], preferred_element_type=jnp.float32)
        for s in range(seqs):
            out_ref[s, :, d * w_cols : (d + 1) * w_cols] = result[s * toks : (s + 1) * toks].astype(
                jnp.bfloat16
            )
    drain(staged.at[0, 0], back_sem, backs)


def on_device(n, m, queries, key_maps, value_rows, gate_logits, mix_lambda, head_gain, out_weight):
    seqs, heads, toks, cols = queries.shape
    items = seqs * heads
    rows = items // (n // 4)
    width = gate_logits.shape[2]
    w_rows, w_cols = out_weight.shape
    anywhere = pl.BlockSpec(memory_space=pl.ANY)
    in_vmem = pl.BlockSpec(memory_space=pltpu.VMEM)
    result = pl.pallas_call(
        functools.partial(layer_kernel, n, m, heads),
        out_shape=jax.ShapeDtypeStruct((seqs, toks, width), jnp.bfloat16),
        in_specs=[
            anywhere, anywhere, anywhere, anywhere, pl.BlockSpec(memory_space=pltpu.SMEM), in_vmem, anywhere,
        ],
        out_specs=in_vmem,
        scratch_shapes=[
            pltpu.VMEM((rows, 3 * n, toks, cols), jnp.bfloat16),
            pltpu.VMEM((rows, n, toks, cols), jnp.bfloat16),
            pltpu.VMEM((items, toks, cols), jnp.bfloat16),
            pltpu.VMEM((m, n * w_rows, w_cols), jnp.bfloat16),
            pltpu.VMEM(gate_logits.shape, jnp.bfloat16),
            pltpu.VMEM((seqs * toks, width), jnp.bfloat16),
            pltpu.SemaphoreType.DMA((rows,)),
            pltpu.SemaphoreType.DMA,
            pltpu.SemaphoreType.DMA,
            pltpu.SemaphoreType.DMA,
            pltpu.SemaphoreType.DMA((n, m)),
            pltpu.SemaphoreType.DMA,
            pltpu.SemaphoreType.DMA,
        ],
        compiler_params=pltpu.CompilerParams(
            collective_id=0, has_side_effects=True, vmem_limit_bytes=60 * 2**20
        ),
        cost_estimate=pl.CostEstimate(flops=5 * 10**10, bytes_accessed=2**28, transcendentals=0),
    )(
        queries.reshape(items, toks, cols),
        key_maps.reshape(items, toks, cols),
        value_rows.reshape(items, toks, cols),
        gate_logits,
        mix_lambda,
        head_gain.reshape(1, cols),
        out_weight,
    )
    return jnp.transpose(result, (1, 0, 2))


def solution(mesh):
    placed = (
        P("dp", None, "sp", None),
        P("dp", None, "sp", None),
        P("dp", None, "sp", None),
        P("sp", "dp", None),
        P(),
        P(),
        P("sp", "dp"),
    )
    return jax.shard_map(
        functools.partial(on_device, mesh.shape["sp"], mesh.shape["dp"]),
        mesh=mesh,
        in_specs=placed,
        out_specs=P("sp", "dp", None),
        check_vma=False,
    )
```

```python
import functools

import jax
import jax.numpy as jnp
from jax import lax
from jax.experimental import pallas as pl
from jax.experimental.pallas import tpu as pltpu
from jax.sharding import PartitionSpec as P

HEAD_DIM = 64
STRETCH = 64
LOG2E = 1.4426950408889634
GROUPS = 8
WINDOW = 16
NEAR = 0
GATE = 1
FAR = 9
SIDE = 17
ACROSS = 25


def plan(n, items):
    rows = items // (n // 4)
    singles = 2 * ((rows * 7) // 32)
    doubles = rows - singles
    outer_single = singles * 2 // 7
    inner_double = doubles // 6
    groups = [
        (outer_single, 0, 0),
        (singles - outer_single, 0, 1),
        (doubles - inner_double, 1, 0),
        (inner_double, 1, 1),
    ]
    order = sorted(
        ((i + 0.5) / count, g) for g, (count, _, _) in enumerate(groups) for i in range(count)
    )
    kinds, lows, highs, seen = [], [], [], 0
    for _, g in order:
        _, kind, low = groups[g]
        kinds.append(kind)
        lows.append(low)
        highs.append(2 + seen % 2)
        seen += kind
    return kinds, lows, highs


def item_at(place, seqs, heads):
    return lax.rem(place, seqs) * heads + place // seqs


def pick(table, index):
    value = jnp.int32(table[0])
    for i, entry in enumerate(table[1:], 1):
        value = jnp.where(index == i, entry, value)
    return value


def attend(q, k, v, start, weight_two, gain, store):
    rows_all, cols = q.shape
    block = min(2 * STRETCH, rows_all)
    factor = HEAD_DIM ** (-0.5) * LOG2E
    first_map = lax.broadcasted_iota(jnp.int32, (block, cols), 1) < cols // 2
    row_seg = (lax.broadcasted_iota(jnp.int32, (2 * block, block), 0) % block) // STRETCH
    col_seg = lax.broadcasted_iota(jnp.int32, (2 * block, block), 1) // STRETCH
    visible = col_seg <= row_seg
    for at in range(0, rows_all, block):
        lo = start + at
        hi = lo + block
        rows = q[at : at + block]
        zero = jnp.zeros_like(rows)
        both = jnp.concatenate([jnp.where(first_map, rows, zero), jnp.where(first_map, zero, rows)], axis=0)
        scores = lax.dot_general(
            both, k[:hi], (((1,), (1,)), ((), ())), preferred_element_type=jnp.float32
        )
        diag = jnp.where(visible, scores[:, lo:], -1e30)
        scores = jnp.concatenate([scores[:, :lo], diag], axis=1) if lo else diag
        highest = jnp.max(scores, axis=1, keepdims=True)
        weights = jnp.exp2((scores - highest) * factor)
        summed = jnp.sum(weights, axis=1, keepdims=True)
        mapped = (
            jnp.dot(weights.astype(jnp.bfloat16), v[:hi], preferred_element_type=jnp.float32) / summed
        )
        combined = mapped[:block] - weight_two * mapped[block:]
        mean_sq = jnp.mean(combined * combined, axis=1, keepdims=True)
        store(at, (combined * lax.rsqrt(mean_sq + 1e-05) * gain).astype(jnp.bfloat16))


def layer_kernel(
    n, m, heads, q_ref, k_ref, v_ref, gate_ref, lam_ref, gain_ref, w_ref, out_ref,
    recv, staged, ret, wbuf, gate_v, gated, partial,
    recv_sem, send_sem, ret_sem, back_sem, w_sem, w_send_sem, gate_sem,
):
    me = lax.axis_index("sp")
    col = lax.axis_index("dp")
    items, toks, cols = q_ref.shape
    seqs = items // heads
    half = n // 2
    quarter = n // 4
    rows = items // quarter
    kinds, lows, highs = plan(n, items)
    low = me < half
    my_quarter = me // quarter
    my_column = lax.rem(me, quarter)
    w_rows, w_cols = w_ref.shape

    cores = 2 if m % 2 == 0 else 1
    xs = m // cores
    ys = 1
    while 2 * (2 * ys) ** 2 <= n:
        ys *= 2
    zs = n // ys
    hz = zs // 2
    my_z, my_y = me // ys, lax.rem(me, ys)
    my_x, my_core = col // cores, lax.rem(col, cores)

    barrier = pltpu.get_barrier_semaphore()

    def greet_sp(step, carry):
        pl.semaphore_signal(barrier, inc=1, device_id={"sp": lax.rem(me + step, n)})
        return carry

    def greet_dp(step, carry):
        pl.semaphore_signal(barrier, inc=1, device_id={"dp": lax.rem(col + step, m)})
        return carry

    gate_copy = pltpu.make_async_copy(gate_ref, gate_v, gate_sem)
    gate_copy.start()
    lax.fori_loop(1, n, greet_sp, 0)
    lax.fori_loop(1, m, greet_dp, 0)

    def w_at(s, d):
        return wbuf.at[d, pl.ds(pl.multiple_of(s * w_rows, w_rows), w_rows)]

    pltpu.make_async_copy(w_ref, w_at(me, col), w_sem.at[me, col]).start()
    pl.semaphore_wait(barrier, n - 1 + m - 1)

    def w_send(src, s, d, **target):
        pltpu.make_async_remote_copy(
            src_ref=src, dst_ref=w_at(s, d), send_sem=w_send_sem, recv_sem=w_sem.at[s, d], device_id=target
        ).start()

    def w_wait(s, d):
        pltpu.make_async_copy(w_at(s, d), w_at(s, d), w_sem.at[s, d]).wait()

    def to_half_peers(src, s, d):
        for i in range(1, hz):
            base = (my_z // hz) * hz
            w_send(src, s, d, sp=(base + lax.rem(my_z - base + i, hz)) * ys + my_y)

    def to_ys(src, s, d):
        for i in range(1, ys):
            w_send(src, s, d, sp=my_z * ys + lax.rem(my_y + i, ys))

    def to_xs(src, s, d):
        for i in range(1, xs):
            w_send(src, s, d, dp=lax.rem(my_x + i, xs) * cores + my_core)

    def to_core(src, s, d):
        if cores > 1:
            w_send(src, s, d, dp=my_x * cores + (1 - my_core))

    base_z = (my_z // hz) * hz
    far_z = hz - base_z
    is_gate = my_z == jnp.where(low, hz - 1, hz)

    w_send(w_ref, me, col, sp=jnp.where(low, hz, hz - 1) * ys + my_y)
    to_half_peers(w_ref, me, col)
    to_ys(w_ref, me, col)
    to_xs(w_ref, me, col)
    to_core(w_ref, me, col)

    def w_near():
        for i in range(1, ys):
            s = my_z * ys + lax.rem(my_y + i, ys)
            w_wait(s, col)
            to_xs(w_at(s, col), s, col)
            to_core(w_at(s, col), s, col)
        for i in range(1, hz):
            s = (base_z + lax.rem(my_z - base_z + i, hz)) * ys + my_y
            w_wait(s, col)
            to_ys(w_at(s, col), s, col)
            to_xs(w_at(s, col), s, col)
            to_core(w_at(s, col), s, col)

    def w_far(gateway):
        for i in range(hz):
            s = (far_z + i) * ys + my_y
            w_wait(s, col)
            if gateway:
                to_half_peers(w_at(s, col), s, col)
            to_ys(w_at(s, col), s, col)
            to_xs(w_at(s, col), s, col)
            to_core(w_at(s, col), s, col)

    def w_side():
        for j in range(1, ys):
            for i in range(1, zs):
                s = lax.rem(my_z + i, zs) * ys + lax.rem(my_y + j, ys)
                w_wait(s, col)
                to_xs(w_at(s, col), s, col)
                to_core(w_at(s, col), s, col)

    def w_across():
        for i in range(1, xs):
            d = lax.rem(my_x + i, xs) * cores + my_core

            def forward(s, carry):
                w_wait(s, d)
                to_core(w_at(s, d), s, d)
                return carry

            lax.fori_loop(0, n, forward, 0)

    def w_last():
        if cores > 1:
            for i in range(xs):
                d = i * cores + (1 - my_core)

                def arrive(s, carry):
                    w_wait(s, d)
                    return carry

                lax.fori_loop(0, n, arrive, 0)
        w_wait(me, col)

    near = 1 + (hz - 1) + (ys - 1) + (xs - 1) + (cores - 1)
    passed = (n - 1) * (xs - 1 + cores - 1) + (zs - 1) * (ys - 1) + n * (xs - 1) * (cores - 1)
    w_sends = near + passed + jnp.where(is_gate, hz * (hz - 1), 0)

    def send_row(r):
        kind, low_q, high_q = pick(kinds, r), pick(lows, r), pick(highs, r)

        def send_item(c, carry):
            item = item_at(r * quarter + c, seqs, heads)
            first = jnp.where((kind == 0) | low, low_q, high_q) * quarter + c

            @pl.when(first == me)
            def _():
                for which, ref in enumerate((q_ref, k_ref, v_ref)):
                    pltpu.make_async_copy(ref.at[item], recv.at[r, which * n + me], recv_sem.at[r]).start()

            def far(which, ref, peer):
                pltpu.make_async_remote_copy(
                    src_ref=ref.at[item],
                    dst_ref=recv.at[r, which * n + me],
                    send_sem=send_sem,
                    recv_sem=recv_sem.at[r],
                    device_id={"sp": peer},
                ).start()

            @pl.when(first != me)
            def _():
                for which, ref in enumerate((q_ref, k_ref, v_ref)):
                    far(which, ref, first)

            @pl.when((kind == 1) & low)
            def _():
                far(1, k_ref, high_q * quarter + c)
                far(2, v_ref, high_q * quarter + c)

            return carry

        lax.fori_loop(0, quarter, send_item, 0)

    def send_first(r, carry):
        send_row(r)
        return carry

    lax.fori_loop(0, min(WINDOW, rows), send_first, 0)

    gate_copy.wait()
    for h in range(heads):
        logits = gate_v[:, :, h * cols : (h + 1) * cols].astype(jnp.float32)
        gated[h] = jax.nn.sigmoid(logits).reshape(toks * seqs, cols)

    gain = gain_ref[...]

    def arrived(part, sem):
        pltpu.make_async_copy(part, part, sem).wait()

    def work_row(r, carry):
        @pl.when(r + WINDOW < rows)
        def _():
            send_row(r + WINDOW)

        @pl.when(r == NEAR * rows // 32)
        def _():
            w_near()

        @pl.when((r == GATE * rows // 32) & is_gate)
        def _():
            w_far(True)

        @pl.when((r == FAR * rows // 32) & jnp.logical_not(is_gate))
        def _():
            w_far(False)

        @pl.when(r == SIDE * rows // 32)
        def _():
            w_side()

        @pl.when(r == ACROSS * rows // 32)
        def _():
            w_across()

        kind, low_q, high_q = pick(kinds, r), pick(lows, r), pick(highs, r)
        place = r * quarter + my_column
        item = item_at(place, seqs, heads)
        group = place // (items // GROUPS)
        weight_two = lam_ref[place // seqs]
        is_low = low & (low_q == my_quarter)
        is_high = jnp.logical_not(low) & (kind == 1) & (high_q == my_quarter)

        def part(first, count):
            q = recv[r, first : first + count].reshape(count * toks, cols)
            k = recv[r, n : n + first + count].reshape((first + count) * toks, cols)
            v = recv[r, 2 * n : 2 * n + first + count].reshape((first + count) * toks, cols)

            def store(at, block):
                for i in range(0, block.shape[0], toks):
                    staged[r, first + (at + i) // toks] = block[i : i + toks]

            attend(q, k, v, first * toks, weight_two, gain, store)
            for s in range(first, first + count):

                @pl.when(me == s)
                def _():
                    pltpu.make_async_copy(staged.at[r, s], ret.at[place], ret_sem.at[group]).start()

                @pl.when(me != s)
                def _():
                    pltpu.make_async_remote_copy(
                        src_ref=staged.at[r, s],
                        dst_ref=ret.at[place],
                        send_sem=back_sem,
                        recv_sem=ret_sem.at[group],
                        device_id={"sp": s},
                    ).start()

        @pl.when(is_low & (kind == 0))
        def _():
            arrived(recv.at[r], recv_sem.at[r])

        @pl.when(is_low & (kind == 1))
        def _():
            arrived(recv.at[r, pl.ds(0, 3 * half)], recv_sem.at[r])

        @pl.when(is_high)
        def _():
            arrived(recv.at[r, pl.ds(half, 3 * n - half)], recv_sem.at[r])

        @pl.when(is_low)
        def _():
            part(0, half)

        @pl.when((is_low & (kind == 0)) | is_high)
        def _():
            part(half, half)

        return carry

    lax.fori_loop(0, rows, work_row, 0)
    w_last()

    n_single = [sum(1 for k, l in zip(kinds, lows) if k == 0 and l == i) for i in range(2)]
    n_double = [sum(1 for k, l in zip(kinds, lows) if k == 1 and l == i) for i in range(2)]
    n_high = [sum(1 for k, h in zip(kinds, highs) if k == 1 and h == i) for i in (2, 3)]
    doubles = sum(kinds) * quarter
    mine = [n_single[i] + n_double[i] for i in range(2)] + n_high
    sent = items - pick(mine, my_quarter)
    backs = pick(
        [mine[i] * (half - 1) + n_single[i] * half for i in range(2)] + [h * (half - 1) for h in n_high],
        my_quarter,
    )

    def drain(part, sem, count):
        def one(i, carry):
            pltpu.make_async_copy(part, part, sem).wait()
            return carry

        lax.fori_loop(0, count, one, 0)

    drain(recv.at[0, pl.ds(0, 3)], send_sem, sent)
    drain(recv.at[0, pl.ds(0, 2)], send_sem, jnp.where(low, doubles, 0))
    drain(w_at(me, col), w_send_sem, w_sends)

    per_group = items // GROUPS

    def gate_group(g):
        part = ret.at[pl.ds(g * per_group, per_group)]
        arrived(part, ret_sem.at[g])
        for place in range(g * per_group, (g + 1) * per_group):
            h, s = place // seqs, place % seqs
            at = (h, pl.ds(s, toks, stride=seqs))
            gated[at] = gated[at] * ret[place].astype(jnp.float32)

    def gated_rows(first, end):
        return jnp.concatenate([gated[h].astype(jnp.bfloat16) for h in range(first, end)], axis=1)

    last_head = heads - heads // GROUPS
    last = last_head * cols
    for g in range(GROUPS - 1):
        gate_group(g)
    for d in range(m):
        partial[:, d * w_cols : (d + 1) * w_cols] = jnp.dot(
            gated_rows(0, last_head), wbuf[d, :last], preferred_element_type=jnp.float32
        )
    gate_group(GROUPS - 1)
    for d in range(m):
        at = slice(d * w_cols, (d + 1) * w_cols)
        result = partial[:, at] + jnp.dot(
            gated_rows(last_head, heads), wbuf[d, last:], preferred_element_type=jnp.float32
        )
        out_ref[:, :, at] = result.astype(jnp.bfloat16).reshape(toks, seqs, w_cols)
    drain(staged.at[0, 0], back_sem, backs)


def on_device(n, m, queries, key_maps, value_rows, gate_logits, mix_lambda, head_gain, out_weight):
    seqs, heads, toks, cols = queries.shape
    items = seqs * heads
    rows = items // (n // 4)
    width = gate_logits.shape[2]
    w_rows, w_cols = out_weight.shape
    anywhere = pl.BlockSpec(memory_space=pl.ANY)
    in_vmem = pl.BlockSpec(memory_space=pltpu.VMEM)
    result = pl.pallas_call(
        functools.partial(layer_kernel, n, m, heads),
        out_shape=jax.ShapeDtypeStruct((toks, seqs, width), jnp.bfloat16),
        in_specs=[
            anywhere, anywhere, anywhere, anywhere, pl.BlockSpec(memory_space=pltpu.SMEM), in_vmem, anywhere,
        ],
        out_specs=in_vmem,
        scratch_shapes=[
            pltpu.VMEM((rows, 3 * n, toks, cols), jnp.bfloat16),
            pltpu.VMEM((rows, n, toks, cols), jnp.bfloat16),
            pltpu.VMEM((items, toks, cols), jnp.bfloat16),
            pltpu.VMEM((m, n * w_rows, w_cols), jnp.bfloat16),
            pltpu.VMEM(gate_logits.shape, jnp.bfloat16),
            pltpu.VMEM((heads, toks * seqs, cols), jnp.float32),
            pltpu.VMEM((toks * seqs, width), jnp.float32),
            pltpu.SemaphoreType.DMA((rows,)),
            pltpu.SemaphoreType.DMA,
            pltpu.SemaphoreType.DMA((GROUPS,)),
            pltpu.SemaphoreType.DMA,
            pltpu.SemaphoreType.DMA((n, m)),
            pltpu.SemaphoreType.DMA,
            pltpu.SemaphoreType.DMA,
        ],
        compiler_params=pltpu.CompilerParams(
            collective_id=0, has_side_effects=True, vmem_limit_bytes=52 * 2**20
        ),
        cost_estimate=pl.CostEstimate(flops=5 * 10**10, bytes_accessed=2**28, transcendentals=0),
    )(
        queries.reshape(items, toks, cols),
        key_maps.reshape(items, toks, cols),
        value_rows.reshape(items, toks, cols),
        gate_logits,
        mix_lambda,
        head_gain.reshape(1, cols),
        out_weight,
    )
    return result


def solution(mesh):
    placed = (
        P("dp", None, "sp", None),
        P("dp", None, "sp", None),
        P("dp", None, "sp", None),
        P("sp", "dp", None),
        P(),
        P(),
        P("sp", "dp"),
    )
    return jax.shard_map(
        functools.partial(on_device, mesh.shape["sp"], mesh.shape["dp"]),
        mesh=mesh,
        in_specs=placed,
        out_specs=P("sp", "dp", None),
        check_vma=False,
    )
```

```python
import functools

import jax
import jax.numpy as jnp
from jax import lax
from jax.experimental import pallas as pl
from jax.experimental.pallas import tpu as pltpu
from jax.sharding import PartitionSpec as P

HEAD_DIM = 64
STRETCH = 64
LOG2E = 1.4426950408889634
GROUPS = 4
WINDOW = 16
NEAR = 0
GATE = 1
FAR = 9
SIDE = 17
ACROSS = 25


def plan(n, items):
    rows = items // (n // 4)
    singles = 2 * ((rows * 7) // 32)
    doubles = rows - singles
    outer_single = singles * 2 // 7
    inner_double = doubles // 6
    groups = [
        (outer_single, 0, 0),
        (singles - outer_single, 0, 1),
        (doubles - inner_double, 1, 0),
        (inner_double, 1, 1),
    ]
    order = sorted(
        ((i + 0.5) / count, g) for g, (count, _, _) in enumerate(groups) for i in range(count)
    )
    kinds, lows, highs, seen = [], [], [], 0
    for _, g in order:
        _, kind, low = groups[g]
        kinds.append(kind)
        lows.append(low)
        highs.append(2 + seen % 2)
        seen += kind
    return kinds, lows, highs


def item_at(place, seqs, heads):
    return lax.rem(place, seqs) * heads + place // seqs


def grid_of(n):
    ys = 1
    while 2 * (2 * ys) ** 2 <= n:
        ys *= 2
    return ys, n // ys


def rounds_of(zs, ys):
    return max(zs - 1 + (ys > 1) - 1, 1)


def pick(table, index):
    value = jnp.int32(table[0])
    for i, entry in enumerate(table[1:], 1):
        value = jnp.where(index == i, entry, value)
    return value


def attend(q, k, v, start, weight_two, gain, store):
    rows_all, cols = q.shape
    block = min(2 * STRETCH, rows_all)
    factor = HEAD_DIM ** (-0.5) * LOG2E
    first_map = lax.broadcasted_iota(jnp.int32, (block, cols), 1) < cols // 2
    row_seg = (lax.broadcasted_iota(jnp.int32, (2 * block, block), 0) % block) // STRETCH
    col_seg = lax.broadcasted_iota(jnp.int32, (2 * block, block), 1) // STRETCH
    visible = col_seg <= row_seg
    for at in range(0, rows_all, block):
        lo = start + at
        hi = lo + block
        rows = q[at : at + block]
        zero = jnp.zeros_like(rows)
        both = jnp.concatenate([jnp.where(first_map, rows, zero), jnp.where(first_map, zero, rows)], axis=0)
        scores = lax.dot_general(
            both, k[:hi], (((1,), (1,)), ((), ())), preferred_element_type=jnp.float32
        )
        diag = jnp.where(visible, scores[:, lo:], -1e30)
        scores = jnp.concatenate([scores[:, :lo], diag], axis=1) if lo else diag
        highest = jnp.max(scores, axis=1, keepdims=True)
        weights = jnp.exp2((scores - highest) * factor)
        summed = jnp.sum(weights, axis=1, keepdims=True)
        mapped = (
            jnp.dot(weights.astype(jnp.bfloat16), v[:hi], preferred_element_type=jnp.float32) / summed
        )
        combined = mapped[:block] - weight_two * mapped[block:]
        mean_sq = jnp.mean(combined * combined, axis=1, keepdims=True)
        store(at, (combined * lax.rsqrt(mean_sq + 1e-05) * gain).astype(jnp.bfloat16))


def layer_kernel(
    n, m, heads, q_ref, k_ref, v_ref, gate_ref, lam_ref, gain_ref, w_ref, out_ref,
    recv, staged, ret, wbuf, gate_v, gated, partial,
    recv_sem, send_sem, ret_sem, back_sem, w_sem, w_send_sem, gate_sem, round_sem,
):
    me = lax.axis_index("sp")
    col = lax.axis_index("dp")
    items, toks, cols = q_ref.shape
    seqs = items // heads
    half = n // 2
    quarter = n // 4
    rows = items // quarter
    kinds, lows, highs = plan(n, items)
    low = me < half
    my_quarter = me // quarter
    my_column = lax.rem(me, quarter)
    w_rows, w_cols = w_ref.shape

    cores = 2 if m % 2 == 0 else 1
    xs = m // cores
    ys, zs = grid_of(n)
    hz = zs // 2
    my_z, my_y = me // ys, lax.rem(me, ys)
    my_x, my_core = col // cores, lax.rem(col, cores)

    barrier = pltpu.get_barrier_semaphore()

    def greet_near(sem):
        @pl.when(my_z > 0)
        def _():
            pl.semaphore_signal(sem, inc=1, device_id={"sp": me - ys})

        @pl.when(my_z < zs - 1)
        def _():
            pl.semaphore_signal(sem, inc=1, device_id={"sp": me + ys})

        for i in range(1, ys):
            pl.semaphore_signal(sem, inc=1, device_id={"sp": my_z * ys + lax.rem(my_y + i, ys)})

    near_count = jnp.where(my_z > 0, 1, 0) + jnp.where(my_z < zs - 1, 1, 0) + ys - 1

    def greet_dp(step, carry):
        pl.semaphore_signal(barrier, inc=1, device_id={"dp": lax.rem(col + step, m)})
        return carry

    gate_copy = pltpu.make_async_copy(gate_ref, gate_v, gate_sem)
    gate_copy.start()
    greet_near(barrier)
    lax.fori_loop(1, m, greet_dp, 0)

    def w_at(s, d):
        return wbuf.at[d, pl.ds(pl.multiple_of(s * w_rows, w_rows), w_rows)]

    pltpu.make_async_copy(w_ref, w_at(me, col), w_sem.at[me, col]).start()
    pl.semaphore_wait(barrier, near_count + m - 1)

    def w_send(src, s, d, **target):
        pltpu.make_async_remote_copy(
            src_ref=src, dst_ref=w_at(s, d), send_sem=w_send_sem, recv_sem=w_sem.at[s, d], device_id=target
        ).start()

    def w_wait(s, d):
        pltpu.make_async_copy(w_at(s, d), w_at(s, d), w_sem.at[s, d]).wait()

    def to_half_peers(src, s, d):
        for i in range(1, hz):
            base = (my_z // hz) * hz
            w_send(src, s, d, sp=(base + lax.rem(my_z - base + i, hz)) * ys + my_y)

    def to_ys(src, s, d):
        for i in range(1, ys):
            w_send(src, s, d, sp=my_z * ys + lax.rem(my_y + i, ys))

    def to_xs(src, s, d):
        for i in range(1, xs):
            w_send(src, s, d, dp=lax.rem(my_x + i, xs) * cores + my_core)

    def to_core(src, s, d):
        if cores > 1:
            w_send(src, s, d, dp=my_x * cores + (1 - my_core))

    base_z = (my_z // hz) * hz
    far_z = hz - base_z
    is_gate = my_z == jnp.where(low, hz - 1, hz)

    def to_gate():
        w_send(w_ref, me, col, sp=jnp.where(low, hz, hz - 1) * ys + my_y)

    greet_near(round_sem.at[0])
    pl.when(is_gate)(to_gate)
    to_ys(w_ref, me, col)
    if hz == 2:
        to_half_peers(w_ref, me, col)
    to_xs(w_ref, me, col)
    to_core(w_ref, me, col)
    pl.semaphore_wait(round_sem.at[0], near_count)
    for i in range(1, rounds_of(zs, ys)):
        greet_near(round_sem.at[i])
        pl.semaphore_wait(round_sem.at[i], near_count)
    pl.when(jnp.logical_not(is_gate))(to_gate)
    if hz != 2:
        to_half_peers(w_ref, me, col)

    def w_near():
        for i in range(1, ys):
            s = my_z * ys + lax.rem(my_y + i, ys)
            w_wait(s, col)
            to_xs(w_at(s, col), s, col)
            to_core(w_at(s, col), s, col)
        for i in range(1, hz):
            s = (base_z + lax.rem(my_z - base_z + i, hz)) * ys + my_y
            w_wait(s, col)
            to_ys(w_at(s, col), s, col)
            to_xs(w_at(s, col), s, col)
            to_core(w_at(s, col), s, col)

    def w_far(gateway):
        for i in range(hz):
            s = (far_z + i) * ys + my_y
            w_wait(s, col)
            if gateway:
                to_half_peers(w_at(s, col), s, col)
            to_ys(w_at(s, col), s, col)
            to_xs(w_at(s, col), s, col)
            to_core(w_at(s, col), s, col)

    def w_side():
        for j in range(1, ys):
            for i in range(1, zs):
                s = lax.rem(my_z + i, zs) * ys + lax.rem(my_y + j, ys)
                w_wait(s, col)
                to_xs(w_at(s, col), s, col)
                to_core(w_at(s, col), s, col)

    def w_across():
        for i in range(1, xs):
            d = lax.rem(my_x + i, xs) * cores + my_core

            def forward(s, carry):
                w_wait(s, d)
                to_core(w_at(s, d), s, d)
                return carry

            lax.fori_loop(0, n, forward, 0)

    def w_last():
        if cores > 1:
            for i in range(xs):
                d = i * cores + (1 - my_core)

                def arrive(s, carry):
                    w_wait(s, d)
                    return carry

                lax.fori_loop(0, n, arrive, 0)
        w_wait(me, col)

    near = 1 + (hz - 1) + (ys - 1) + (xs - 1) + (cores - 1)
    passed = (n - 1) * (xs - 1 + cores - 1) + (zs - 1) * (ys - 1) + n * (xs - 1) * (cores - 1)
    w_sends = near + passed + jnp.where(is_gate, hz * (hz - 1), 0)

    def send_row(r):
        kind, low_q, high_q = pick(kinds, r), pick(lows, r), pick(highs, r)

        def send_item(c, carry):
            item = item_at(r * quarter + c, seqs, heads)
            first = jnp.where((kind == 0) | low, low_q, high_q) * quarter + c

            @pl.when(first == me)
            def _():
                for which, ref in enumerate((q_ref, k_ref, v_ref)):
                    pltpu.make_async_copy(ref.at[item], recv.at[r, which * n + me], recv_sem.at[r]).start()

            def far(which, ref, peer):
                pltpu.make_async_remote_copy(
                    src_ref=ref.at[item],
                    dst_ref=recv.at[r, which * n + me],
                    send_sem=send_sem,
                    recv_sem=recv_sem.at[r],
                    device_id={"sp": peer},
                ).start()

            @pl.when(first != me)
            def _():
                for which, ref in enumerate((q_ref, k_ref, v_ref)):
                    far(which, ref, first)

            @pl.when((kind == 1) & low)
            def _():
                far(1, k_ref, high_q * quarter + c)
                far(2, v_ref, high_q * quarter + c)

            return carry

        lax.fori_loop(0, quarter, send_item, 0)

    def send_first(r, carry):
        send_row(r)
        return carry

    lax.fori_loop(0, min(WINDOW, rows), send_first, 0)

    gate_copy.wait()
    for h in range(heads):
        logits = gate_v[:, :, h * cols : (h + 1) * cols].astype(jnp.float32)
        gated[h] = jax.nn.sigmoid(logits).reshape(toks * seqs, cols)

    gain = gain_ref[...]

    def arrived(part, sem):
        pltpu.make_async_copy(part, part, sem).wait()

    def work_row(r, carry):
        @pl.when(r + WINDOW < rows)
        def _():
            send_row(r + WINDOW)

        @pl.when(r == NEAR * rows // 32)
        def _():
            w_near()

        @pl.when((r == GATE * rows // 32) & is_gate)
        def _():
            w_far(True)

        @pl.when((r == FAR * rows // 32) & jnp.logical_not(is_gate))
        def _():
            w_far(False)

        @pl.when(r == SIDE * rows // 32)
        def _():
            w_side()

        @pl.when(r == ACROSS * rows // 32)
        def _():
            w_across()

        kind, low_q, high_q = pick(kinds, r), pick(lows, r), pick(highs, r)
        place = r * quarter + my_column
        item = item_at(place, seqs, heads)
        group = place // (items // GROUPS)
        weight_two = lam_ref[place // seqs]
        is_low = low & (low_q == my_quarter)
        is_high = jnp.logical_not(low) & (kind == 1) & (high_q == my_quarter)

        def part(first, count):
            q = recv[r, first : first + count].reshape(count * toks, cols)
            k = recv[r, n : n + first + count].reshape((first + count) * toks, cols)
            v = recv[r, 2 * n : 2 * n + first + count].reshape((first + count) * toks, cols)

            def give_back(s):
                @pl.when(me == s)
                def _():
                    pltpu.make_async_copy(staged.at[r, s], ret.at[place], ret_sem.at[group]).start()

                @pl.when(me != s)
                def _():
                    pltpu.make_async_remote_copy(
                        src_ref=staged.at[r, s],
                        dst_ref=ret.at[place],
                        send_sem=back_sem,
                        recv_sem=ret_sem.at[group],
                        device_id={"sp": s},
                    ).start()

            def store(at, block):
                for i in range(0, block.shape[0], toks):
                    staged[r, first + (at + i) // toks] = block[i : i + toks]
                for i in range(0, block.shape[0], toks):
                    give_back(first + (at + i) // toks)

            attend(q, k, v, first * toks, weight_two, gain, store)

        @pl.when(is_low & (kind == 0))
        def _():
            arrived(recv.at[r], recv_sem.at[r])

        @pl.when(is_low & (kind == 1))
        def _():
            arrived(recv.at[r, pl.ds(0, 3 * half)], recv_sem.at[r])

        @pl.when(is_high)
        def _():
            arrived(recv.at[r, pl.ds(half, 3 * n - half)], recv_sem.at[r])

        @pl.when(is_low)
        def _():
            part(0, half)

        @pl.when((is_low & (kind == 0)) | is_high)
        def _():
            part(half, half)

        return carry

    lax.fori_loop(0, rows, work_row, 0)
    w_last()

    n_single = [sum(1 for k, l in zip(kinds, lows) if k == 0 and l == i) for i in range(2)]
    n_double = [sum(1 for k, l in zip(kinds, lows) if k == 1 and l == i) for i in range(2)]
    n_high = [sum(1 for k, h in zip(kinds, highs) if k == 1 and h == i) for i in (2, 3)]
    doubles = sum(kinds) * quarter
    mine = [n_single[i] + n_double[i] for i in range(2)] + n_high
    sent = items - pick(mine, my_quarter)
    backs = pick(
        [mine[i] * (half - 1) + n_single[i] * half for i in range(2)] + [h * (half - 1) for h in n_high],
        my_quarter,
    )

    def drain(part, sem, count):
        def one(i, carry):
            pltpu.make_async_copy(part, part, sem).wait()
            return carry

        lax.fori_loop(0, count, one, 0)

    drain(recv.at[0, pl.ds(0, 3)], send_sem, sent)
    drain(recv.at[0, pl.ds(0, 2)], send_sem, jnp.where(low, doubles, 0))
    drain(w_at(me, col), w_send_sem, w_sends)

    per_group = items // GROUPS

    def gate_group(g):
        part = ret.at[pl.ds(g * per_group, per_group)]
        arrived(part, ret_sem.at[g])
        for place in range(g * per_group, (g + 1) * per_group):
            h, s = place // seqs, place % seqs
            at = (h, pl.ds(s, toks, stride=seqs))
            gated[at] = gated[at] * ret[place].astype(jnp.float32)

    def gated_rows(first, end):
        return jnp.concatenate([gated[h].astype(jnp.bfloat16) for h in range(first, end)], axis=1)

    last_head = heads - heads // GROUPS
    last = last_head * cols
    for g in range(GROUPS - 1):
        gate_group(g)
    for d in range(m):
        partial[:, d * w_cols : (d + 1) * w_cols] = jnp.dot(
            gated_rows(0, last_head), wbuf[d, :last], preferred_element_type=jnp.float32
        )
    gate_group(GROUPS - 1)
    for d in range(m):
        at = slice(d * w_cols, (d + 1) * w_cols)
        result = partial[:, at] + jnp.dot(
            gated_rows(last_head, heads), wbuf[d, last:], preferred_element_type=jnp.float32
        )
        out_ref[:, :, at] = result.astype(jnp.bfloat16).reshape(toks, seqs, w_cols)
    drain(staged.at[0, 0], back_sem, backs)


def on_device(n, m, queries, key_maps, value_rows, gate_logits, mix_lambda, head_gain, out_weight):
    seqs, heads, toks, cols = queries.shape
    items = seqs * heads
    rows = items // (n // 4)
    width = gate_logits.shape[2]
    w_rows, w_cols = out_weight.shape
    ys, zs = grid_of(n)
    anywhere = pl.BlockSpec(memory_space=pl.ANY)
    in_vmem = pl.BlockSpec(memory_space=pltpu.VMEM)
    result = pl.pallas_call(
        functools.partial(layer_kernel, n, m, heads),
        out_shape=jax.ShapeDtypeStruct((toks, seqs, width), jnp.bfloat16),
        in_specs=[
            anywhere, anywhere, anywhere, anywhere, pl.BlockSpec(memory_space=pltpu.SMEM), in_vmem, anywhere,
        ],
        out_specs=in_vmem,
        scratch_shapes=[
            pltpu.VMEM((rows, 3 * n, toks, cols), jnp.bfloat16),
            pltpu.VMEM((rows, n, toks, cols), jnp.bfloat16),
            pltpu.VMEM((items, toks, cols), jnp.bfloat16),
            pltpu.VMEM((m, n * w_rows, w_cols), jnp.bfloat16),
            pltpu.VMEM(gate_logits.shape, jnp.bfloat16),
            pltpu.VMEM((heads, toks * seqs, cols), jnp.float32),
            pltpu.VMEM((toks * seqs, width), jnp.float32),
            pltpu.SemaphoreType.DMA((rows,)),
            pltpu.SemaphoreType.DMA,
            pltpu.SemaphoreType.DMA((GROUPS,)),
            pltpu.SemaphoreType.DMA,
            pltpu.SemaphoreType.DMA((n, m)),
            pltpu.SemaphoreType.DMA,
            pltpu.SemaphoreType.DMA,
            pltpu.SemaphoreType.REGULAR((rounds_of(zs, ys),)),
        ],
        compiler_params=pltpu.CompilerParams(
            collective_id=0, has_side_effects=True, vmem_limit_bytes=52 * 2**20
        ),
        cost_estimate=pl.CostEstimate(flops=5 * 10**10, bytes_accessed=2**28, transcendentals=0),
    )(
        queries.reshape(items, toks, cols),
        key_maps.reshape(items, toks, cols),
        value_rows.reshape(items, toks, cols),
        gate_logits,
        mix_lambda,
        head_gain.reshape(1, cols),
        out_weight,
    )
    return result


def solution(mesh):
    placed = (
        P("dp", None, "sp", None),
        P("dp", None, "sp", None),
        P("dp", None, "sp", None),
        P("sp", "dp", None),
        P(),
        P(),
        P("sp", "dp"),
    )
    return jax.shard_map(
        functools.partial(on_device, mesh.shape["sp"], mesh.shape["dp"]),
        mesh=mesh,
        in_specs=placed,
        out_specs=P("sp", "dp", None),
        check_vma=False,
    )
```

```python
import functools

import jax
import jax.numpy as jnp
from jax import lax
from jax.experimental import pallas as pl
from jax.experimental.pallas import tpu as pltpu
from jax.sharding import PartitionSpec as P

HEAD_DIM = 64
STRETCH = 64
LOG2E = 1.4426950408889634
GROUPS = 4
WINDOW = 16
NEAR = 0
GATE = 0
FAR = 9
BESIDE = 13
SIDE = 17
ACROSS = 25


def plan(n, items):
    rows = items // (n // 4)
    singles = 2 * ((rows * 7) // 32)
    doubles = rows - singles
    outer_single = singles * 2 // 7
    inner_double = doubles // 6
    groups = [
        (outer_single, 0, 0),
        (singles - outer_single, 0, 1),
        (doubles - inner_double, 1, 0),
        (inner_double, 1, 1),
    ]
    order = sorted(
        ((i + 0.5) / count, g) for g, (count, _, _) in enumerate(groups) for i in range(count)
    )
    kinds, lows, highs, seen = [], [], [], 0
    for _, g in order:
        _, kind, low = groups[g]
        kinds.append(kind)
        lows.append(low)
        highs.append(2 + seen % 2)
        seen += kind
    return kinds, lows, highs


def item_at(place, seqs, heads):
    return lax.rem(place, seqs) * heads + place // seqs


def grid_of(n):
    ys = 1
    while 2 * (2 * ys) ** 2 <= n:
        ys *= 2
    return ys, n // ys


def rounds_of(zs, ys):
    return max(zs - 1 + (ys > 1) - 1, 1)


def pick(table, index):
    value = jnp.int32(table[0])
    for i, entry in enumerate(table[1:], 1):
        value = jnp.where(index == i, entry, value)
    return value


def attend(q, k, v, start, weight_two, gain, store):
    rows_all, cols = q.shape
    block = min(2 * STRETCH, rows_all)
    factor = HEAD_DIM ** (-0.5) * LOG2E
    first_map = lax.broadcasted_iota(jnp.int32, (block, cols), 1) < cols // 2
    row_seg = (lax.broadcasted_iota(jnp.int32, (2 * block, block), 0) % block) // STRETCH
    col_seg = lax.broadcasted_iota(jnp.int32, (2 * block, block), 1) // STRETCH
    visible = col_seg <= row_seg
    for at in range(0, rows_all, block):
        lo = start + at
        hi = lo + block
        rows = q[at : at + block]
        zero = jnp.zeros_like(rows)
        both = jnp.concatenate([jnp.where(first_map, rows, zero), jnp.where(first_map, zero, rows)], axis=0)
        scores = lax.dot_general(
            both, k[:hi], (((1,), (1,)), ((), ())), preferred_element_type=jnp.float32
        )
        diag = jnp.where(visible, scores[:, lo:], -1e30)
        scores = jnp.concatenate([scores[:, :lo], diag], axis=1) if lo else diag
        highest = jnp.max(scores, axis=1, keepdims=True)
        weights = jnp.exp2((scores - highest) * factor)
        summed = jnp.sum(weights, axis=1, keepdims=True)
        mapped = (
            jnp.dot(weights.astype(jnp.bfloat16), v[:hi], preferred_element_type=jnp.float32) / summed
        )
        combined = mapped[:block] - weight_two * mapped[block:]
        mean_sq = jnp.mean(combined * combined, axis=1, keepdims=True)
        store(at, (combined * lax.rsqrt(mean_sq + 1e-05) * gain).astype(jnp.bfloat16))


def layer_kernel(
    n, m, heads, q_ref, k_ref, v_ref, gate_ref, lam_ref, gain_ref, w_ref, out_ref,
    recv, staged, ret, wbuf, gate_v, gated, partial,
    recv_sem, send_sem, ret_sem, back_sem, w_sem, w_send_sem, gate_sem, round_sem,
):
    me = lax.axis_index("sp")
    col = lax.axis_index("dp")
    items, toks, cols = q_ref.shape
    seqs = items // heads
    half = n // 2
    quarter = n // 4
    rows = items // quarter
    kinds, lows, highs = plan(n, items)
    low = me < half
    my_quarter = me // quarter
    my_column = lax.rem(me, quarter)
    w_rows, w_cols = w_ref.shape

    cores = 2 if m % 2 == 0 else 1
    xs = m // cores
    ys, zs = grid_of(n)
    hz = zs // 2
    my_z, my_y = me // ys, lax.rem(me, ys)
    my_x, my_core = col // cores, lax.rem(col, cores)

    barrier = pltpu.get_barrier_semaphore()

    def greet_near(sem):
        @pl.when(my_z > 0)
        def _():
            pl.semaphore_signal(sem, inc=1, device_id={"sp": me - ys})

        @pl.when(my_z < zs - 1)
        def _():
            pl.semaphore_signal(sem, inc=1, device_id={"sp": me + ys})

        for i in range(1, ys):
            pl.semaphore_signal(sem, inc=1, device_id={"sp": my_z * ys + lax.rem(my_y + i, ys)})

    near_count = jnp.where(my_z > 0, 1, 0) + jnp.where(my_z < zs - 1, 1, 0) + ys - 1

    def greet_dp(step, carry):
        pl.semaphore_signal(barrier, inc=1, device_id={"dp": lax.rem(col + step, m)})
        return carry

    gate_copy = pltpu.make_async_copy(gate_ref, gate_v, gate_sem)
    gate_copy.start()
    greet_near(barrier)
    lax.fori_loop(1, m, greet_dp, 0)

    def w_at(s, d):
        return wbuf.at[d, pl.ds(pl.multiple_of(s * w_rows, w_rows), w_rows)]

    pltpu.make_async_copy(w_ref, w_at(me, col), w_sem.at[me, col]).start()
    pl.semaphore_wait(barrier, near_count + m - 1)

    def w_send(src, s, d, **target):
        pltpu.make_async_remote_copy(
            src_ref=src, dst_ref=w_at(s, d), send_sem=w_send_sem, recv_sem=w_sem.at[s, d], device_id=target
        ).start()

    def w_wait(s, d):
        pltpu.make_async_copy(w_at(s, d), w_at(s, d), w_sem.at[s, d]).wait()

    def to_half_peers(src, s, d):
        for i in range(1, hz):
            base = (my_z // hz) * hz
            w_send(src, s, d, sp=(base + lax.rem(my_z - base + i, hz)) * ys + my_y)

    def to_ys(src, s, d):
        for i in range(1, ys):
            w_send(src, s, d, sp=my_z * ys + lax.rem(my_y + i, ys))

    def to_xs(src, s, d):
        for i in range(1, xs):
            w_send(src, s, d, dp=lax.rem(my_x + i, xs) * cores + my_core)

    def to_core(src, s, d):
        if cores > 1:
            w_send(src, s, d, dp=my_x * cores + (1 - my_core))

    base_z = (my_z // hz) * hz
    far_z = hz - base_z
    is_gate = my_z == jnp.where(low, hz - 1, hz)

    def to_gate():
        w_send(w_ref, me, col, sp=jnp.where(low, hz, hz - 1) * ys + my_y)

    greet_near(round_sem.at[0])
    pl.when(is_gate)(to_gate)
    to_ys(w_ref, me, col)
    if hz == 2:
        to_half_peers(w_ref, me, col)
    to_xs(w_ref, me, col)
    to_core(w_ref, me, col)
    pl.semaphore_wait(round_sem.at[0], near_count)
    for i in range(1, rounds_of(zs, ys)):
        greet_near(round_sem.at[i])
        pl.semaphore_wait(round_sem.at[i], near_count)
    pl.when(jnp.logical_not(is_gate))(to_gate)
    if hz != 2:
        to_half_peers(w_ref, me, col)

    def w_near():
        for i in range(1, ys):
            s = my_z * ys + lax.rem(my_y + i, ys)
            w_wait(s, col)
            to_xs(w_at(s, col), s, col)
            to_core(w_at(s, col), s, col)
        for i in range(1, hz):
            s = (base_z + lax.rem(my_z - base_z + i, hz)) * ys + my_y
            w_wait(s, col)
            to_ys(w_at(s, col), s, col)
            to_xs(w_at(s, col), s, col)
            to_core(w_at(s, col), s, col)

    def w_far(gateway):
        for i in range(hz):
            s = (far_z + i) * ys + my_y
            w_wait(s, col)
            if gateway:
                to_half_peers(w_at(s, col), s, col)
            to_ys(w_at(s, col), s, col)
            to_xs(w_at(s, col), s, col)
            to_core(w_at(s, col), s, col)

    def w_side(own_half):
        for j in range(1, ys):
            for i in range(1 if own_half else 0, hz):
                z = base_z + lax.rem(my_z - base_z + i, hz) if own_half else far_z + i
                s = z * ys + lax.rem(my_y + j, ys)
                w_wait(s, col)
                to_xs(w_at(s, col), s, col)
                to_core(w_at(s, col), s, col)

    def w_across():
        for i in range(1, xs):
            d = lax.rem(my_x + i, xs) * cores + my_core

            def forward(s, carry):
                w_wait(s, d)
                to_core(w_at(s, d), s, d)
                return carry

            lax.fori_loop(0, n, forward, 0)

    def w_last():
        if cores > 1:
            for i in range(xs):
                d = i * cores + (1 - my_core)

                def arrive(s, carry):
                    w_wait(s, d)
                    return carry

                lax.fori_loop(0, n, arrive, 0)
        w_wait(me, col)

    near = 1 + (hz - 1) + (ys - 1) + (xs - 1) + (cores - 1)
    passed = (n - 1) * (xs - 1 + cores - 1) + (zs - 1) * (ys - 1) + n * (xs - 1) * (cores - 1)
    w_sends = near + passed + jnp.where(is_gate, hz * (hz - 1), 0)

    def send_row(r):
        kind, low_q, high_q = pick(kinds, r), pick(lows, r), pick(highs, r)

        def send_item(step, carry):
            c = lax.rem(step + my_column, quarter)
            item = item_at(r * quarter + c, seqs, heads)
            first = jnp.where((kind == 0) | low, low_q, high_q) * quarter + c

            @pl.when(first == me)
            def _():
                for which, ref in enumerate((q_ref, k_ref, v_ref)):
                    pltpu.make_async_copy(ref.at[item], recv.at[r, which * n + me], recv_sem.at[r]).start()

            def far(which, ref, peer):
                pltpu.make_async_remote_copy(
                    src_ref=ref.at[item],
                    dst_ref=recv.at[r, which * n + me],
                    send_sem=send_sem,
                    recv_sem=recv_sem.at[r],
                    device_id={"sp": peer},
                ).start()

            @pl.when(first != me)
            def _():
                for which, ref in enumerate((q_ref, k_ref, v_ref)):
                    far(which, ref, first)

            @pl.when((kind == 1) & low)
            def _():
                far(1, k_ref, high_q * quarter + c)
                far(2, v_ref, high_q * quarter + c)

            return carry

        lax.fori_loop(0, quarter, send_item, 0)

    def send_first(r, carry):
        send_row(r)
        return carry

    lax.fori_loop(0, min(WINDOW, rows), send_first, 0)

    gate_copy.wait()
    for h in range(heads):
        logits = gate_v[:, :, h * cols : (h + 1) * cols].astype(jnp.float32)
        gated[h] = jax.nn.sigmoid(logits).reshape(toks * seqs, cols)

    gain = gain_ref[...]

    def arrived(part, sem):
        pltpu.make_async_copy(part, part, sem).wait()

    def work_row(r, carry):
        @pl.when(r + WINDOW < rows)
        def _():
            send_row(r + WINDOW)

        @pl.when(r == NEAR * rows // 32)
        def _():
            w_near()

        @pl.when((r == GATE * rows // 32) & is_gate)
        def _():
            w_far(True)

        @pl.when((r == FAR * rows // 32) & jnp.logical_not(is_gate))
        def _():
            w_far(False)

        @pl.when(r == BESIDE * rows // 32)
        def _():
            w_side(True)

        @pl.when(r == SIDE * rows // 32)
        def _():
            w_side(False)

        @pl.when(r == ACROSS * rows // 32)
        def _():
            w_across()

        kind, low_q, high_q = pick(kinds, r), pick(lows, r), pick(highs, r)
        place = r * quarter + my_column
        item = item_at(place, seqs, heads)
        group = place // (items // GROUPS)
        weight_two = lam_ref[place // seqs]
        is_low = low & (low_q == my_quarter)
        is_high = jnp.logical_not(low) & (kind == 1) & (high_q == my_quarter)

        def part(first, count):
            q = recv[r, first : first + count].reshape(count * toks, cols)
            k = recv[r, n : n + first + count].reshape((first + count) * toks, cols)
            v = recv[r, 2 * n : 2 * n + first + count].reshape((first + count) * toks, cols)

            def give_back(s):
                @pl.when(me == s)
                def _():
                    pltpu.make_async_copy(staged.at[r, s], ret.at[place], ret_sem.at[group]).start()

                @pl.when(me != s)
                def _():
                    pltpu.make_async_remote_copy(
                        src_ref=staged.at[r, s],
                        dst_ref=ret.at[place],
                        send_sem=back_sem,
                        recv_sem=ret_sem.at[group],
                        device_id={"sp": s},
                    ).start()

            def store(at, block):
                for i in range(0, block.shape[0], toks):
                    staged[r, first + (at + i) // toks] = block[i : i + toks]
                for i in range(0, block.shape[0], toks):
                    give_back(first + (at + i) // toks)

            attend(q, k, v, first * toks, weight_two, gain, store)

        @pl.when(is_low & (kind == 0))
        def _():
            arrived(recv.at[r], recv_sem.at[r])

        @pl.when(is_low & (kind == 1))
        def _():
            arrived(recv.at[r, pl.ds(0, 3 * half)], recv_sem.at[r])

        @pl.when(is_high)
        def _():
            arrived(recv.at[r, pl.ds(half, 3 * n - half)], recv_sem.at[r])

        @pl.when(is_low)
        def _():
            part(0, half)

        @pl.when((is_low & (kind == 0)) | is_high)
        def _():
            part(half, half)

        return carry

    lax.fori_loop(0, rows, work_row, 0)
    w_last()

    n_single = [sum(1 for k, l in zip(kinds, lows) if k == 0 and l == i) for i in range(2)]
    n_double = [sum(1 for k, l in zip(kinds, lows) if k == 1 and l == i) for i in range(2)]
    n_high = [sum(1 for k, h in zip(kinds, highs) if k == 1 and h == i) for i in (2, 3)]
    doubles = sum(kinds) * quarter
    mine = [n_single[i] + n_double[i] for i in range(2)] + n_high
    sent = items - pick(mine, my_quarter)
    backs = pick(
        [mine[i] * (half - 1) + n_single[i] * half for i in range(2)] + [h * (half - 1) for h in n_high],
        my_quarter,
    )

    def drain(part, sem, count):
        def one(i, carry):
            pltpu.make_async_copy(part, part, sem).wait()
            return carry

        lax.fori_loop(0, count, one, 0)

    drain(recv.at[0, pl.ds(0, 3)], send_sem, sent)
    drain(recv.at[0, pl.ds(0, 2)], send_sem, jnp.where(low, doubles, 0))
    drain(w_at(me, col), w_send_sem, w_sends)

    per_group = items // GROUPS

    def gate_group(g):
        part = ret.at[pl.ds(g * per_group, per_group)]
        arrived(part, ret_sem.at[g])
        for place in range(g * per_group, (g + 1) * per_group):
            h, s = place // seqs, place % seqs
            at = (h, pl.ds(s, toks, stride=seqs))
            gated[at] = gated[at] * ret[place].astype(jnp.float32)

    def gated_rows(first, end):
        return jnp.concatenate([gated[h].astype(jnp.bfloat16) for h in range(first, end)], axis=1)

    last_head = heads - heads // GROUPS
    last = last_head * cols
    for g in range(GROUPS - 1):
        gate_group(g)
    for d in range(m):
        partial[:, d * w_cols : (d + 1) * w_cols] = jnp.dot(
            gated_rows(0, last_head), wbuf[d, :last], preferred_element_type=jnp.float32
        )
    gate_group(GROUPS - 1)
    for d in range(m):
        at = slice(d * w_cols, (d + 1) * w_cols)
        result = partial[:, at] + jnp.dot(
            gated_rows(last_head, heads), wbuf[d, last:], preferred_element_type=jnp.float32
        )
        out_ref[:, :, at] = result.astype(jnp.bfloat16).reshape(toks, seqs, w_cols)
    drain(staged.at[0, 0], back_sem, backs)


def on_device(n, m, queries, key_maps, value_rows, gate_logits, mix_lambda, head_gain, out_weight):
    seqs, heads, toks, cols = queries.shape
    items = seqs * heads
    rows = items // (n // 4)
    width = gate_logits.shape[2]
    w_rows, w_cols = out_weight.shape
    ys, zs = grid_of(n)
    anywhere = pl.BlockSpec(memory_space=pl.ANY)
    in_vmem = pl.BlockSpec(memory_space=pltpu.VMEM)
    result = pl.pallas_call(
        functools.partial(layer_kernel, n, m, heads),
        out_shape=jax.ShapeDtypeStruct((toks, seqs, width), jnp.bfloat16),
        in_specs=[
            anywhere, anywhere, anywhere, anywhere, pl.BlockSpec(memory_space=pltpu.SMEM), in_vmem, anywhere,
        ],
        out_specs=in_vmem,
        scratch_shapes=[
            pltpu.VMEM((rows, 3 * n, toks, cols), jnp.bfloat16),
            pltpu.VMEM((rows, n, toks, cols), jnp.bfloat16),
            pltpu.VMEM((items, toks, cols), jnp.bfloat16),
            pltpu.VMEM((m, n * w_rows, w_cols), jnp.bfloat16),
            pltpu.VMEM(gate_logits.shape, jnp.bfloat16),
            pltpu.VMEM((heads, toks * seqs, cols), jnp.float32),
            pltpu.VMEM((toks * seqs, width), jnp.float32),
            pltpu.SemaphoreType.DMA((rows,)),
            pltpu.SemaphoreType.DMA,
            pltpu.SemaphoreType.DMA((GROUPS,)),
            pltpu.SemaphoreType.DMA,
            pltpu.SemaphoreType.DMA((n, m)),
            pltpu.SemaphoreType.DMA,
            pltpu.SemaphoreType.DMA,
            pltpu.SemaphoreType.REGULAR((rounds_of(zs, ys),)),
        ],
        compiler_params=pltpu.CompilerParams(
            collective_id=0, has_side_effects=True, vmem_limit_bytes=52 * 2**20
        ),
        cost_estimate=pl.CostEstimate(flops=5 * 10**10, bytes_accessed=2**28, transcendentals=0),
    )(
        queries.reshape(items, toks, cols),
        key_maps.reshape(items, toks, cols),
        value_rows.reshape(items, toks, cols),
        gate_logits,
        mix_lambda,
        head_gain.reshape(1, cols),
        out_weight,
    )
    return result


def solution(mesh):
    placed = (
        P("dp", None, "sp", None),
        P("dp", None, "sp", None),
        P("dp", None, "sp", None),
        P("sp", "dp", None),
        P(),
        P(),
        P("sp", "dp"),
    )
    return jax.shard_map(
        functools.partial(on_device, mesh.shape["sp"], mesh.shape["dp"]),
        mesh=mesh,
        in_specs=placed,
        out_specs=P("sp", "dp", None),
        check_vma=False,
    )
```
